128 devices in a mesh: row: 16 (over z, x), col: 8 (over y, core).
Axes of the slice: x: 4, y: 4, z: 4, core: 2. Of those that a mesh axis runs over, the one named last changes fastest.
Arguments:
- tokens: bfloat16 [65536, 4096], P(('row', 'col')), may hold values from -36 to 36
- norm_gain: bfloat16 [4096], replicated, may hold values from 0.099609375 to 1.8984375
- in_weight: bfloat16 [4096, 1024], replicated, may hold values from -0.09375 to 0.09375
- out_weight: bfloat16 [1024, 4096], replicated, may hold values from -0.1875 to 0.1875
Outputs:
- mixed: bfloat16 [65536, 4096], P(('row', 'col'))
The draws below stay inside these ranges and needn't reach their ends.
All inputs are finite; a program needn't handle non-finite values.
Results may differ from the reference program's by a relative error of at most 0.0071.
Values may be sent and summed in bfloat16 or wider, within the bound.
A program may use at most 128 MiB of HBM per device.

```python
import jax
import jax.numpy as jnp
from jax import lax

D = 4096
GROUP_WIDTH = 64
F = 1024
TOKENS = 65536


def draw_tokens(key, part):
    keys = jax.random.split(key, 3)
    base = jnp.clip(jax.random.normal(keys[0], (TOKENS, D), jnp.float32), -4.0, 4.0)
    row_scales = jnp.exp(jax.random.uniform(keys[1], (TOKENS, 1), jnp.float32, -1.2, 1.0986))
    col_scales = jnp.exp(jax.random.uniform(keys[2], (1, D), jnp.float32, -1.2, 1.0986))
    return (base * row_scales * col_scales).astype(jnp.bfloat16)


def scatter_about(rng, extent, spread, limit, held_as=jnp.bfloat16):
    return jnp.clip(spread * jax.random.normal(rng, extent, jnp.float32), -limit, limit).astype(held_as)


def setup_inputs(seed: int = 0) -> dict:
    streams_of = jax.random.split(jax.random.key(seed), 5)
    return {
        "tokens": draw_tokens(jax.random.fold_in(streams_of[4], 71), 0),
        "norm_gain": jnp.clip(1.0 + 0.18 * jax.random.normal(streams_of[1], (D,), jnp.float32), 0.099609375, 1.8984375).astype(jnp.bfloat16),
        "in_weight": scatter_about(streams_of[2], (D, F), D ** -0.5, 0.09375),
        "out_weight": scatter_about(streams_of[3], (F, D), F ** -0.5, 0.1875),
    }


def reference(tokens, norm_gain, in_weight, out_weight):
    floats = tokens.astype(jnp.float32)
    scaling = lax.rsqrt(lax.optimization_barrier(jnp.mean(floats * floats, axis=-1, keepdims=True)) + 1e-06)
    normed = (floats * scaling * norm_gain.astype(jnp.float32)).astype(jnp.bfloat16)
    hidden = jnp.dot(normed, in_weight, preferred_element_type=jnp.float32).astype(jnp.bfloat16)
    widened = lax.optimization_barrier(hidden).astype(jnp.float32)
    length = widened.shape[0]
    grouped = widened.reshape(length, widened.shape[1] // GROUP_WIDTH, GROUP_WIDTH)
    channel_spectrum = jnp.fft.fft(grouped, axis=2, norm='ortho')
    real_rounded = channel_spectrum.real.astype(jnp.bfloat16)
    imag_rounded = channel_spectrum.imag.astype(jnp.bfloat16)
    real_rounded, imag_rounded = lax.optimization_barrier((real_rounded, imag_rounded))
    combined = real_rounded.astype(jnp.float32) + 1j * imag_rounded.astype(jnp.float32)
    spectrum = jnp.fft.fft(combined, axis=0, norm='ortho').real
    spectrum = spectrum.reshape(length, widened.shape[1]).astype(jnp.bfloat16)
    return jnp.dot(spectrum, out_weight, preferred_element_type=jnp.float32).astype(jnp.bfloat16)
```

```python
import functools
import math

import jax
import jax.numpy as jnp
import numpy as np
from jax import lax
from jax.experimental import pallas as pl
from jax.experimental.pallas import tpu as pltpu
from jax.sharding import PartitionSpec as P

ROWS = 512
WIDTH = 4096
PLANES = 4
PER = 32
CH = 8
MESH = pl.DeviceIdType.MESH
F32 = jnp.float32
BF16 = jnp.bfloat16


def channel_table():
    table = np.zeros((256, 256))
    c = np.arange(64)
    for g in range(4):
        for i in range(8):
            for ch in range(8):
                p = 4 * i + ch % 4
                if ch < 4:
                    row = np.cos(2 * np.pi * c * p / 64)
                elif p == 0:
                    row = np.cos(np.pi * c)
                else:
                    row = -np.sin(2 * np.pi * c * p / 64)
                table[g * 64 + i * 8 + ch, g * 64 : g * 64 + 64] = row / 8
    return table


def unpack_table():
    table = np.zeros((256, 256))
    for g in range(4):
        for i in range(8):
            for ch in range(4):
                p = 4 * i + ch
                real, imag = g * 64 + i * 8 + ch, g * 64 + i * 8 + ch + 4
                if p == 0:
                    table[real, g * 64] = 1
                    table[imag, g * 64 + 32] = 1
                else:
                    table[real, g * 64 + p] = 1
                    table[imag, g * 64 + p] = 1
                    table[real, g * 64 + 64 - p] = 1
                    table[imag, g * 64 + 64 - p] = -1
    return table


def swap_table():
    table = np.zeros((256, 256))
    for d in range(PER):
        for ch in range(CH):
            table[ch * PER + d, d * CH + ch] = 1
    return table


def tables():
    chan = channel_table()
    high = chan.astype(BF16)
    low = (chan - high.astype(np.float64)).astype(BF16)
    swap = swap_table()
    square = np.concatenate([high, low, swap.astype(BF16), swap.T.astype(BF16), unpack_table().astype(BF16)])
    d = np.arange(128)
    angle = 2 * np.pi * ((d[:, None] * d[None, :]) % 128) / 128
    outer = np.concatenate([np.cos(angle), -np.sin(angle)]).astype(BF16)
    j = np.arange(512)
    twist = 2 * np.pi * (d[:, None] * j[None, :]) / 65536
    twist = np.stack([np.cos(twist), np.sin(twist)]).astype(np.float32)
    e = np.arange(128).reshape(4, 1, 32)
    s = np.arange(4).reshape(1, 4, 1)
    p = (4 * e + s).reshape(512)
    angle = 2 * np.pi * ((p[:, None] * j[None, :]) % 512) / 512
    inner = (np.concatenate([np.cos(angle), np.sin(angle)], axis=1) / 256).astype(BF16)
    return square.reshape(5, 256, 256), outer, twist, inner


def coords(device):
    return {"row": device // 8, "col": device % 8}


def mixer(
    tok_hbm, gain_ref, win_hbm, square_hbm, outer_hbm, twist_hbm, inner_hbm, spec_ref,
    tok, win, square, outer, twist, inner, send1, recv1, send2, recv2, xb, ts,
    tok_sem, win_sem, tab_sem, ssem1, rsem1, ssem2, rsem2,
):
    me = lax.axis_index("row") * 8 + lax.axis_index("col")
    plane = me // PER
    place = me % PER

    barrier = pltpu.get_barrier_semaphore()

    @pl.loop(1, 128)
    def _(r):
        pl.semaphore_signal(barrier, 1, device_id=coords((me + r) % 128), device_id_type=MESH)

    tok_copies = []
    for i in range(8):
        rows = pl.ds(i * 64, 64)
        copy = pltpu.make_async_copy(tok_hbm.at[rows], tok.at[rows], tok_sem.at[i])
        copy.start()
        tok_copies.append(copy)
    win_copies = []
    for tt in range(PLANES):
        target = (plane + 1 + tt) % PLANES
        copy = pltpu.make_async_copy(
            win_hbm.at[:, pl.ds(pl.multiple_of(target * 256, 256), 256)], win.at[tt], win_sem.at[tt]
        )
        copy.start()
        win_copies.append(copy)
    tab_copies = []
    for i, (a, b) in enumerate(
        ((square_hbm, square), (outer_hbm, outer), (twist_hbm, twist), (inner_hbm, inner))
    ):
        copy = pltpu.make_async_copy(a, b, tab_sem.at[i])
        copy.start()
        tab_copies.append(copy)

    gain = gain_ref[...].astype(F32)
    for i in range(8):
        tok_copies[i].wait()

        @pl.loop(0, 4)
        def _(k):
            rows = pl.ds(pl.multiple_of(i * 64 + k * 16, 16), 16)
            x = tok[rows, :].astype(F32)
            scale = lax.rsqrt(jnp.mean(x * x, axis=-1, keepdims=True) + 1e-06)
            tok[rows, :] = (x * scale * gain).astype(BF16)

    tab_copies[0].wait()
    pl.semaphore_wait(barrier, 127)

    for tt in range(PLANES):
        target = (plane + 1 + tt) % PLANES
        win_copies[tt].wait()
        h = jnp.dot(tok[...], win[tt], preferred_element_type=F32).astype(BF16)
        dims = (((1,), (1,)), ((), ()))
        s = lax.dot_general(square[0], h, dims, preferred_element_type=F32) + lax.dot_general(
            square[1], h, dims, preferred_element_type=F32
        )
        send1[pl.ds(target * PER, PER)] = s.reshape(PER, CH, ROWS).astype(BF16)
        if tt == PLANES - 1:
            recv1[me] = send1[me]

        @pl.loop(1 if tt == PLANES - 1 else 0, PER)
        def _(r):
            dest = target * PER + (place + r) % PER
            pltpu.make_async_remote_copy(
                send1.at[dest], recv1.at[me], ssem1, rsem1.at[plane], device_id=coords(dest), device_id_type=MESH
            ).start()

    for copy in tab_copies[1:]:
        copy.wait()

    def wait_block(send, recv, sem, source, count):
        pltpu.make_async_remote_copy(
            send.at[pl.ds(0, count)], recv.at[pl.ds(0, count)], sem, sem, device_id=coords(me), device_id_type=MESH
        ).wait_recv()

    for tt in range(PLANES):
        source = (plane + 3 - tt) % PLANES
        wait_block(send1, recv1, rsem1.at[source], source, PER - (tt == PLANES - 1))
        block = recv1[pl.ds(source * PER, PER)].reshape(PER * CH, ROWS)
        x = jnp.dot(square[2], block, preferred_element_type=F32).astype(BF16)
        for ch in range(CH):
            xb[ch, pl.ds(pl.multiple_of(source * PER, PER), PER), :] = x[ch * PER : ch * PER + PER]

    special = place % 8 == 0
    for cp in range(4):
        parts = []
        for ch in (2 * cp, 2 * cp + 1):
            a = jnp.dot(outer[...], xb[ch], preferred_element_type=F32)
            re, im = a[:128], a[128:]
            b_re = re * twist[0] + im * twist[1]
            b_im = im * twist[0] - re * twist[1]
            if ch == 4:
                b_re, b_im = jnp.where(special, b_re, -b_im), jnp.where(special, b_im, b_re)
            elif ch > 4:
                b_re, b_im = -b_im, b_re
            parts.append(jnp.concatenate([b_re.astype(BF16), b_im.astype(BF16)], axis=1))
        b = jnp.concatenate(parts, axis=0)
        t = lax.dot_general(inner[...], b, (((1,), (1,)), ((), ())), preferred_element_type=F32)
        for eb in range(4):
            for s in range(4):
                for c in range(2):
                    ch = 2 * cp + c
                    ts[eb, ch * PER : ch * PER + PER, s * 128 : s * 128 + 128] = t[
                        (eb * 4 + s) * PER : (eb * 4 + s + 1) * PER, c * 128 : c * 128 + 128
                    ].astype(BF16)

    for tt in range(PLANES):
        target = (plane + 1 + tt) % PLANES
        y = jnp.dot(square[3], ts[target], preferred_element_type=F32)
        send2[pl.ds(target * PER, PER)] = y.reshape(PER, CH, ROWS).astype(BF16)
        if tt == PLANES - 1:
            recv2[me] = send2[me]

        @pl.loop(1 if tt == PLANES - 1 else 0, PER)
        def _(r):
            dest = target * PER + (place + r) % PER
            pltpu.make_async_remote_copy(
                send2.at[dest], recv2.at[me], ssem2, rsem2.at[plane], device_id=coords(dest), device_id_type=MESH
            ).start()

    for tt in range(PLANES):
        source = (plane + 3 - tt) % PLANES
        wait_block(send2, recv2, rsem2.at[source], source, PER - (tt == PLANES - 1))
        block = recv2[pl.ds(source * PER, PER)].reshape(PER * CH, ROWS)
        y = lax.dot_general(block, square[4], (((0,), (0,)), ((), ())), preferred_element_type=F32)
        spec_ref[:, pl.ds(pl.multiple_of(source * 256, 256), 256)] = y.astype(BF16)

    for send, sem in ((send1, ssem1), (send2, ssem2)):
        pltpu.make_async_remote_copy(
            send.at[pl.ds(0, 127)], send.at[pl.ds(0, 127)], sem, sem, device_id=coords(me), device_id_type=MESH
        ).wait_send()


def local(tokens, norm_gain, in_weight, out_weight):
    square, outer, twist, inner = tables()
    hbm = pl.BlockSpec(memory_space=pl.ANY)
    vmem = pl.BlockSpec(memory_space=pltpu.VMEM)
    block = pltpu.VMEM((128, CH, ROWS), BF16)
    spec = pl.pallas_call(
        mixer,
        out_shape=jax.ShapeDtypeStruct((ROWS, 1024), BF16),
        in_specs=[hbm, vmem, hbm, hbm, hbm, hbm, hbm],
        out_specs=vmem,
        scratch_shapes=[
            pltpu.VMEM((ROWS, WIDTH), BF16),
            pltpu.VMEM((PLANES, WIDTH, 256), BF16),
            pltpu.VMEM((5, 256, 256), BF16),
            pltpu.VMEM((256, 128), BF16),
            pltpu.VMEM((2, 128, 512), F32),
            pltpu.VMEM((512, 1024), BF16),
            block, block, block, block,
            pltpu.VMEM((CH, 128, 512), BF16),
            pltpu.VMEM((4, 256, 512), BF16),
            pltpu.SemaphoreType.DMA((8,)),
            pltpu.SemaphoreType.DMA((4,)),
            pltpu.SemaphoreType.DMA((4,)),
            pltpu.SemaphoreType.DMA,
            pltpu.SemaphoreType.DMA((4,)),
            pltpu.SemaphoreType.DMA,
            pltpu.SemaphoreType.DMA((4,)),
        ],
        compiler_params=pltpu.CompilerParams(
            collective_id=0, has_side_effects=True, vmem_limit_bytes=50 * 2**20
        ),
        name="mixer",
    )(tokens, norm_gain.reshape(1, WIDTH), in_weight, jnp.asarray(square), jnp.asarray(outer), jnp.asarray(twist), jnp.asarray(inner))
    mixed = jnp.dot(spec, out_weight, preferred_element_type=F32)
    return mixed.astype(BF16)


def solution(mesh):
    placed = (P(("row", "col"), None), P(), P(), P())
    return jax.shard_map(
        local, mesh=mesh, in_specs=placed, out_specs=P(("row", "col"), None), check_vma=False
    )
```

```python
import functools
import math

import jax
import jax.numpy as jnp
import numpy as np
from jax import lax
from jax.experimental import pallas as pl
from jax.experimental.pallas import tpu as pltpu
from jax.sharding import PartitionSpec as P

ROWS = 512
WIDTH = 4096
PLANES = 4
PER = 32
HALF = 256
MESH = pl.DeviceIdType.MESH
F32 = jnp.float32
BF16 = jnp.bfloat16
LAST = (((1,), (1,)), ((), ()))
FIRST = (((0,), (0,)), ((), ()))


def slot_pair(half, i, slot):
    return 4 * i + 2 * half + slot % 2


def channel_table():
    table = np.zeros((2, 2, 4, 8, 2, 4, 256))
    c = np.arange(64)
    for half in range(2):
        for g in range(4):
            for i in range(8):
                for slot in range(4):
                    p = slot_pair(half, i, slot)
                    if slot < 2:
                        row = np.cos(2 * np.pi * c * p / 64)
                    elif p == 0:
                        row = np.cos(np.pi * c)
                    else:
                        row = -np.sin(2 * np.pi * c * p / 64)
                    for h in range(2):
                        table[h, half, g, i, h, slot, g * 64 : g * 64 + 64] = row / 8
    return table.reshape(2, 512, 256)


def weight_table():
    table = np.zeros((2, 4, 4, 8, 4, 64))
    for half in range(2):
        for g in range(4):
            for i in range(8):
                for slot in range(4):
                    p = slot_pair(half, i, slot)
                    if p == 0:
                        table[half, slot, g, i, g, 0 if slot < 2 else 32] = 1
                    else:
                        table[half, slot, g, i, g, p] = 1
                        table[half, slot, g, i, g, 64 - p] = 1 if slot < 2 else -1
    return table.reshape(256, 256)


def swap_table():
    table = np.zeros((256, 256))
    for d in range(PER):
        for slot in range(8):
            table[slot * PER + d, d * 8 + slot] = 1
    return table


def tables():
    chan = channel_table()
    high = chan.astype(BF16)
    low = (chan - high.astype(np.float64)).astype(BF16)
    chan = np.stack([high, low])
    swap = swap_table()
    square = np.stack([swap, swap.T, weight_table()]).astype(BF16)
    d = np.arange(128)
    angle = 2 * np.pi * ((d[:, None] * d[None, :]) % 128) / 128
    outer = np.concatenate([np.cos(angle), -np.sin(angle)]).astype(BF16)
    j = np.arange(512)
    e = np.arange(128).reshape(4, 1, 32)
    s = np.arange(4).reshape(1, 4, 1)
    p = (4 * e + s).reshape(512)
    angle = 2 * np.pi * ((p[:, None] * j[None, :]) % 512) / 512
    inner = (np.concatenate([np.cos(angle), np.sin(angle)], axis=1) / 256).astype(BF16)
    return chan, square, outer, inner


def series(first, count):
    return [
        (-1) ** k * (2 * math.pi) ** (2 * k + first) / math.factorial(2 * k + first) for k in range(count)
    ]


def polynomial(t, coefficients):
    total = jnp.full_like(t, coefficients[-1])
    for c in coefficients[-2::-1]:
        total = total * t + c
    return total


STEPS = [
    (x, y, c)
    for x, y in sorted(
        ((x, y) for x in range(4) for y in range(4)), key=lambda s: -min(s[0], 4 - s[0]) - min(s[1], 4 - s[1])
    )
    for c in (1, 0)
]


def when(condition, action):
    if isinstance(condition, bool):
        if condition:
            action()
    else:
        pl.when(condition)(action)


def plane_step(tt):
    high, low = tt // 2, tt % 2
    return 2 - low + high - 2 * low * high


def mixer(
    tok_hbm, gain_hbm, win_hbm, wout_hbm, chan_hbm, square_hbm, outer_hbm, inner_hbm,
    acc, spec_b, wmix_b,
    tok, gain_ref, win, wout, wmix_a, chan, square, outer, twist, inner,
    hs, send, recv, xb, ts, spec_a,
    tok_sem, win_sem, tab_sem, ssem, rsem,
):
    row, col = lax.axis_index("row"), lax.axis_index("col")
    me = row * 8 + col
    plane, x = lax.div(row, 4), lax.rem(row, 4)
    y, core = lax.div(col, 2), lax.rem(col, 2)
    xs = [lax.rem(x + i, 4) for i in range(4)]
    cols = [[lax.rem(y + i, 4) * 2 + (core if c == 0 else 1 - core) for c in range(2)] for i in range(4)]

    gain_copy = pltpu.make_async_copy(gain_hbm, gain_ref, tab_sem.at[0])
    gain_copy.start()
    tok_copies = []
    for i in range(8):
        rows = pl.ds(i * 64, 64)
        copy = pltpu.make_async_copy(tok_hbm.at[rows], tok.at[rows], tok_sem.at[i])
        tok_copies.append(copy)

    def win_copy(tt):
        target = lax.rem(plane + plane_step(tt), 4)
        columns = pl.ds(pl.multiple_of(target * 256, 256), 256)
        return pltpu.make_async_copy(win_hbm.at[:, columns], win.at[tt], win_sem.at[tt])

    copies = {}
    for i, (name, a, b) in enumerate(
        (
            ("chan", chan_hbm, chan), ("square", square_hbm, square), ("outer", outer_hbm, outer),
            ("inner", inner_hbm, inner), ("wout", wout_hbm, wout),
        )
    ):
        copies[name] = pltpu.make_async_copy(a, b, tab_sem.at[i + 1])
    for i in range(3):
        tok_copies[i].start()
    win_copy(0).start()
    for i in range(3, 8):
        tok_copies[i].start()
    barrier = pltpu.get_barrier_semaphore()

    @pl.loop(0, 16)
    def _(d):
        to_row = lax.rem(plane + 2 + lax.div(d, 4), 4) * 4 + lax.rem(x + d, 4)
        for dy in range(4):
            for dc in range(2):
                to_col = cols[dy][dc]

                def signal():
                    pl.semaphore_signal(barrier, 1, device_id={"row": to_row, "col": to_col}, device_id_type=MESH)

                if dy == 0 and dc == 0:
                    pl.when(to_row != row)(signal)
                else:
                    signal()

    gain_copy.wait()
    gain = gain_ref[...].astype(F32).reshape(1, WIDTH)

    def first_tile(k):
        rows = slice(k * 128, k * 128 + 128)
        hs[0, rows, :] = jnp.dot(tok[rows, :], win[0], preferred_element_type=F32).astype(BF16)

    for i in range(4):
        tok_copies[2 * i].wait()
        tok_copies[2 * i + 1].wait()
        if i == 1:
            win_copy(0).wait()
        if i > 0:
            first_tile(i - 1)
        for k in range(2):
            rows = slice(i * 128 + k * 64, i * 128 + k * 64 + 64)
            v = tok[rows, :].astype(F32)
            scale = lax.rsqrt(jnp.mean(v * v, axis=-1, keepdims=True) + 1e-06)
            tok[rows, :] = (v * scale * gain).astype(BF16)
        if i == 0:
            copies["chan"].start()
            win_copy(1).start()
        if i == 1:
            win_copy(2).start()
            win_copy(3).start()
    first_tile(3)
    copies["chan"].wait()
    for name in ("wout", "square", "outer", "inner"):
        copies[name].start()

    def exchange(stage, half, tt):
        target = lax.rem(plane + plane_step(tt), 4)
        src, dst = send.at[stage, half], recv.at[stage, half]
        for step in STEPS:
            dx, dy, dc = step
            to_row, to_col = target * 4 + xs[dx], cols[dy][dc]

            def start():
                pltpu.make_async_remote_copy(
                    src.at[to_row * 8 + to_col], dst.at[me], ssem.at[stage, half], rsem.at[stage, half, plane],
                    device_id={"row": to_row, "col": to_col}, device_id_type=MESH,
                ).start()

            if step == (0, 0, 0):
                when(tt != PLANES - 1, start)
            else:
                start()

        def keep():
            recv[stage, half, me] = send[stage, half, me]

        when(tt == PLANES - 1, keep)

    def arrive(stage, half, tt):
        source = lax.rem(plane + 4 - plane_step(tt), 4)

        def wait(count):
            ref = recv.at[stage, half, pl.ds(0, count)]
            pltpu.make_async_remote_copy(
                ref, ref, ssem.at[stage, half], rsem.at[stage, half, source],
                device_id={"row": row, "col": col}, device_id_type=MESH,
            ).wait_recv()

        when(tt != PLANES - 1, lambda: wait(PER))
        when(tt == PLANES - 1, lambda: wait(PER - 1))
        return source

    def block_of(stage, half, source):
        return recv[stage, half, pl.ds(source * PER, PER)].reshape(256, HALF)

    def channels(half, tt):
        target = lax.rem(plane + plane_step(tt), 4)
        rows = pl.ds(half * 256, 256)
        v = sum(
            lax.dot_general(
                chan[part, j, rows], hs[tt, j * HALF : j * HALF + HALF], LAST, preferred_element_type=F32
            )
            for j in range(2)
            for part in range(2)
        )
        send[0, half, pl.ds(target * PER, PER)] = v.reshape(PER, 8, HALF).astype(BF16)

    channels(0, 0)
    pl.semaphore_wait(barrier, 127)
    exchange(0, 0, 0)

    @pl.loop(1, PLANES)
    def _(tt):
        win_copy(tt).wait()
        hs[tt] = jnp.dot(tok[...], win[tt], preferred_element_type=F32).astype(BF16)
        channels(0, tt)
        exchange(0, 0, tt)

    @pl.loop(0, PLANES)
    def _(tt):
        channels(1, tt)
        exchange(0, 1, tt)

    @pl.loop(0, 8)
    def _(i):
        rows = pl.ds(pl.multiple_of(i * 16, 16), 16)
        q = lax.broadcasted_iota(jnp.int32, (16, ROWS), 0) + i * 16
        j = lax.broadcasted_iota(jnp.int32, (16, ROWS), 1)
        turns = (q * j).astype(F32) * (1.0 / 65536) - 0.5
        square_turns = turns * turns
        twist[0, rows, :] = -polynomial(square_turns, series(0, 11))
        twist[1, rows, :] = -polynomial(square_turns, series(1, 11)) * turns

    for name in ("square", "outer", "inner"):
        copies[name].wait()

    special = lax.rem(me, 8) == 0
    for half in range(2):

        @pl.loop(0, PLANES)
        def _(tt):
            source = arrive(0, half, tt)
            v = jnp.dot(square[0], block_of(0, half, source), preferred_element_type=F32).astype(BF16)
            for h in range(2):
                for slot in range(4):
                    xb[slot, pl.ds(pl.multiple_of(source * PER, PER), PER), h * HALF : h * HALF + HALF] = v[
                        (h * 4 + slot) * PER : (h * 4 + slot + 1) * PER
                    ]

        for cp in range(2):
            parts = []
            for slot in (2 * cp, 2 * cp + 1):
                a = jnp.dot(outer[...], xb[slot], preferred_element_type=F32)
                re, im = a[:128], a[128:]
                b_re = re * twist[0] + im * twist[1]
                b_im = im * twist[0] - re * twist[1]
                if half == 0 and slot == 2:
                    b_re, b_im = jnp.where(special, b_re, -b_im), jnp.where(special, b_im, b_re)
                elif slot >= 2:
                    b_re, b_im = -b_im, b_re
                parts.append(jnp.concatenate([b_re.astype(BF16), b_im.astype(BF16)], axis=1))
            b = jnp.concatenate(parts, axis=0)
            t = lax.dot_general(inner[...], b, LAST, preferred_element_type=F32)
            for eb in range(4):
                for s in range(4):
                    for c in range(2):
                        place = (s // 2) * 4 + 2 * cp + c
                        ts[eb, place * PER : place * PER + PER, s % 2 * 128 : s % 2 * 128 + 128] = t[
                            (eb * 4 + s) * PER : (eb * 4 + s + 1) * PER, c * 128 : c * 128 + 128
                        ].astype(BF16)

        @pl.loop(0, PLANES)
        def _(tt):
            target = lax.rem(plane + plane_step(tt), 4)
            v = jnp.dot(square[1], ts[target], preferred_element_type=F32)
            send[1, half, pl.ds(target * PER, PER)] = v.reshape(PER, 8, HALF).astype(BF16)
            exchange(1, half, tt)

    copies["wout"].wait()

    @pl.loop(0, PLANES)
    def _(z):
        rows = pl.ds(pl.multiple_of(z * 256, 256), 256)
        half_rows = pl.ds(pl.multiple_of(z * 128, 128), 128)

        @pl.loop(0, 1)
        def _(n):
            columns = pl.ds(pl.multiple_of(n * 4096, 4096), 4096)
            w = jnp.dot(square[2], wout[rows, columns], preferred_element_type=F32).astype(BF16)
            wmix_a[half_rows, columns] = w[:128]
            wmix_b[half_rows, columns] = w[128:]

    for half, spec in enumerate((spec_a, spec_b)):
        for tt in range(PLANES):
            arrive(1, half, tt)
        for z in range(PLANES):
            v = lax.dot_general(block_of(1, half, z), square[1], FIRST, preferred_element_type=F32).astype(BF16)
            spec[:HALF, z * 128 : z * 128 + 128] = v[:, :128]
            spec[HALF:, z * 128 : z * 128 + 128] = v[:, 128:]

        if half == 0:
            @pl.loop(0, 4)
            def _(n):
                columns = pl.ds(pl.multiple_of(n * 1024, 1024), 1024)
                acc[:, columns] = jnp.dot(spec_a[...], wmix_a[:, columns], preferred_element_type=F32)

    for stage in range(2):
        for half in range(2):
            ref = send.at[stage, half, pl.ds(0, 127)]
            pltpu.make_async_remote_copy(
                ref, ref, ssem.at[stage, half], rsem.at[stage, half, 0],
                device_id={"row": row, "col": col}, device_id_type=MESH,
            ).wait_send()


def finish(acc, spec_b, wmix_b, out_hbm, buf, sem):
    copies = []
    for n in range(8):
        columns = pl.ds(n * 512, 512)
        v = jnp.dot(spec_b[...], wmix_b[:, columns], preferred_element_type=F32)
        buf[n] = (acc[:, columns] + v).astype(BF16)
        copies.append(pltpu.make_async_copy(buf.at[n], out_hbm.at[:, columns], sem.at[n]))
        copies[n].start()
    for copy in copies:
        copy.wait()


def local(tokens, norm_gain, in_weight, out_weight):
    constants = [pltpu.with_memory_space_constraint(jnp.asarray(t), pltpu.HBM) for t in tables()]
    tokens, norm_gain, in_weight, out_weight = (
        pltpu.with_memory_space_constraint(a, pltpu.HBM) for a in (tokens, norm_gain, in_weight, out_weight)
    )
    hbm = pl.BlockSpec(memory_space=pltpu.HBM)
    vmem = pl.BlockSpec(memory_space=pltpu.VMEM)
    acc, spec_b, wmix_b = pl.pallas_call(
        mixer,
        out_shape=[
            jax.ShapeDtypeStruct((ROWS, WIDTH), F32),
            jax.ShapeDtypeStruct((ROWS, 512), BF16),
            jax.ShapeDtypeStruct((512, WIDTH), BF16),
        ],
        in_specs=[hbm] * 8,
        out_specs=[vmem] * 3,
        scratch_shapes=[
            pltpu.VMEM((ROWS, WIDTH), BF16),
            pltpu.VMEM((WIDTH,), BF16),
            pltpu.VMEM((PLANES, WIDTH, 256), BF16),
            pltpu.VMEM((1024, WIDTH), BF16),
            pltpu.VMEM((512, WIDTH), BF16),
            pltpu.VMEM((2, 2, 512, 256), BF16),
            pltpu.VMEM((3, 256, 256), BF16),
            pltpu.VMEM((256, 128), BF16),
            pltpu.VMEM((2, 128, 512), F32),
            pltpu.VMEM((512, 1024), BF16),
            pltpu.VMEM((PLANES, ROWS, 256), BF16),
            pltpu.VMEM((2, 2, 128, 8, HALF), BF16),
            pltpu.VMEM((2, 2, 128, 8, HALF), BF16),
            pltpu.VMEM((4, 128, 512), BF16),
            pltpu.VMEM((4, 256, HALF), BF16),
            pltpu.VMEM((ROWS, 512), BF16),
            pltpu.SemaphoreType.DMA((8,)),
            pltpu.SemaphoreType.DMA((4,)),
            pltpu.SemaphoreType.DMA((7,)),
            pltpu.SemaphoreType.DMA((2, 2)),
            pltpu.SemaphoreType.DMA((2, 2, 4)),
        ],
        compiler_params=pltpu.CompilerParams(
            collective_id=0, has_side_effects=True, vmem_limit_bytes=MIXER_VMEM
        ),
        name="mixer",
    )(tokens, norm_gain, in_weight, out_weight, *constants)
    return pl.pallas_call(
        finish,
        out_shape=jax.ShapeDtypeStruct((ROWS, WIDTH), BF16),
        in_specs=[vmem] * 3,
        out_specs=hbm,
        scratch_shapes=[pltpu.VMEM((8, ROWS, 512), BF16), pltpu.SemaphoreType.DMA((8,))],
        compiler_params=pltpu.CompilerParams(vmem_limit_bytes=FINISH_VMEM),
        name="finish",
    )(acc, spec_b, wmix_b)


MIXER_VMEM = 40 * 2**20
FINISH_VMEM = 8 * 2**20


def solution(mesh):
    placed = (P(("row", "col"), None), P(), P(), P())
    return jax.shard_map(
        local, mesh=mesh, in_specs=placed, out_specs=P(("row", "col"), None), check_vma=False
    )
```

```python
import math
import random

import jax
import jax.numpy as jnp
import numpy as np
from jax import lax
from jax.experimental import pallas as pl
from jax.experimental.pallas import tpu as pltpu
from jax.sharding import PartitionSpec as P

ROWS = 512
WIDTH = 4096
PLANES = 4
PER = 32
HALF = 256
MESH = pl.DeviceIdType.MESH
F32 = jnp.float32
BF16 = jnp.bfloat16
LAST = (((1,), (1,)), ((), ()))
FIRST = (((0,), (0,)), ((), ()))


def slot_pair(half, i, slot):
    return 4 * i + 2 * half + slot % 2


def channel_table():
    table = np.zeros((2, 2, 4, 8, 2, 4, 256))
    c = np.arange(64)
    for half in range(2):
        for g in range(4):
            for i in range(8):
                for slot in range(4):
                    p = slot_pair(half, i, slot)
                    if slot < 2:
                        row = np.cos(2 * np.pi * c * p / 64)
                    elif p == 0:
                        row = np.cos(np.pi * c)
                    else:
                        row = -np.sin(2 * np.pi * c * p / 64)
                    for h in range(2):
                        table[h, half, g, i, h, slot, g * 64 : g * 64 + 64] = row / 8
    return table.reshape(2, 512, 256)


def weight_table():
    table = np.zeros((2, 4, 4, 8, 4, 64))
    for half in range(2):
        for g in range(4):
            for i in range(8):
                for slot in range(4):
                    p = slot_pair(half, i, slot)
                    if p == 0:
                        table[half, slot, g, i, g, 0 if slot < 2 else 32] = 1
                    else:
                        table[half, slot, g, i, g, p] = 1
                        table[half, slot, g, i, g, 64 - p] = 1 if slot < 2 else -1
    return table.reshape(256, 256)


def swap_table():
    table = np.zeros((256, 256))
    for d in range(PER):
        for slot in range(8):
            table[slot * PER + d, d * 8 + slot] = 1
    return table


def tables():
    chan = channel_table()
    high = chan.astype(BF16)
    low = (chan - high.astype(np.float64)).astype(BF16)
    chan = np.stack([high, low])
    swap = swap_table()
    square = np.stack([swap, swap.T, weight_table()]).astype(BF16)
    d = np.arange(128)
    angle = 2 * np.pi * ((d[:, None] * d[None, :]) % 128) / 128
    outer = np.concatenate([np.cos(angle), -np.sin(angle)])
    outer_high = outer.astype(BF16)
    outer = np.concatenate([outer_high, (outer - outer_high.astype(np.float64)).astype(BF16)], axis=1)
    j = np.arange(512)
    e = np.arange(128).reshape(4, 1, 32)
    s = np.arange(4).reshape(1, 4, 1)
    p = (4 * e + s).reshape(512)
    angle = 2 * np.pi * ((p[:, None] * j[None, :]) % 512) / 512
    inner = (np.concatenate([np.cos(angle), np.sin(angle)], axis=1) / 256).astype(BF16)
    return chan, square, outer, inner


def series(first, count):
    return [
        (-1) ** k * (2 * math.pi) ** (2 * k + first) / math.factorial(2 * k + first) for k in range(count)
    ]


def polynomial(t, coefficients):
    total = jnp.full_like(t, coefficients[-1])
    for c in coefficients[-2::-1]:
        total = total * t + c
    return total


def hops(*steps):
    return sum(min(s, 4 - s) for s in steps)


EVERY = [
    (a, b, c, d) for a in range(4) for b in range(4) for c in range(4) for d in range(2) if (a, b, c, d) != (0, 0, 0, 0)
]
random.Random(2).shuffle(EVERY)
EVERY.sort(key=lambda s: -hops(*s[:3]))
STEPS = [(b, c, d) for b in range(4) for c in range(4) for d in range(2) if (b, c, d) != (0, 0, 0)]
random.Random(3).shuffle(STEPS)
STEPS.sort(key=lambda s: -hops(*s[:2]))
STEPS.append((0, 0, 0))


def when(condition, action):
    if isinstance(condition, bool):
        if condition:
            action()
    else:
        pl.when(condition)(action)


def plane_step(tt):
    high, low = tt // 2, tt % 2
    return 2 - low + high - 2 * low * high


def mixer(
    tok_hbm, gain_hbm, win_hbm, wout_hbm, chan_hbm, square_hbm, outer_hbm, inner_hbm,
    acc, spec_b, wmix_b,
    tok, gain_ref, win, wout, wmix_a, chan, square, outer, twist, inner,
    hs, send, recv, xb, ts, spec_a,
    tok_sem, win_sem, tab_sem, ssem, rsem,
):
    row, col = lax.axis_index("row"), lax.axis_index("col")
    me = row * 8 + col
    plane, x = lax.div(row, 4), lax.rem(row, 4)
    y, core = lax.div(col, 2), lax.rem(col, 2)
    planes = [lax.rem(plane + i, 4) for i in range(4)]
    xs = [lax.rem(x + i, 4) for i in range(4)]
    cols = [[lax.rem(y + i, 4) * 2 + (core if c == 0 else 1 - core) for c in range(2)] for i in range(4)]

    gain_copy = pltpu.make_async_copy(gain_hbm, gain_ref, tab_sem.at[0])
    gain_copy.start()
    tok_copies = []
    for i in range(8):
        rows = pl.ds(i * 64, 64)
        copy = pltpu.make_async_copy(tok_hbm.at[rows], tok.at[rows], tok_sem.at[i])
        tok_copies.append(copy)

    def win_copy(tt):
        target = lax.rem(plane + plane_step(tt), 4)
        columns = pl.ds(pl.multiple_of(target * 256, 256), 256)
        return pltpu.make_async_copy(win_hbm.at[:, columns], win.at[tt], win_sem.at[tt])

    copies = {}
    for i, (name, a, b) in enumerate(
        (
            ("chan", chan_hbm, chan), ("square", square_hbm, square), ("outer", outer_hbm, outer),
            ("inner", inner_hbm, inner), ("wout", wout_hbm, wout),
        )
    ):
        copies[name] = pltpu.make_async_copy(a, b, tab_sem.at[i + 1])
    for i in range(3):
        tok_copies[i].start()
    win_copy(0).start()
    for i in range(3, 8):
        tok_copies[i].start()
    barrier = pltpu.get_barrier_semaphore()

    @pl.loop(0, 16)
    def _(d):
        to_row = lax.rem(plane + 2 + lax.div(d, 4), 4) * 4 + lax.rem(x + d, 4)
        for dy in range(4):
            for dc in range(2):
                to_col = cols[dy][dc]

                def signal():
                    pl.semaphore_signal(barrier, 1, device_id={"row": to_row, "col": to_col}, device_id_type=MESH)

                if dy == 0 and dc == 0:
                    pl.when(to_row != row)(signal)
                else:
                    signal()

    gain_copy.wait()
    gain = gain_ref[...].astype(F32).reshape(1, WIDTH)

    for i in range(8):
        tok_copies[i].wait()
        rows = slice(i * 64, i * 64 + 64)
        v = tok[rows, :].astype(F32)
        scale = lax.rsqrt(jnp.mean(v * v, axis=-1, keepdims=True) + 1e-06)
        tok[rows, :] = (v * scale * gain).astype(BF16)
        if i == 1:
            copies["chan"].start()
            win_copy(1).start()
        if i == 3:
            win_copy(2).start()
            win_copy(3).start()
    win_copy(0).wait()
    hs[0] = jnp.dot(tok[...], win[0], preferred_element_type=F32).astype(BF16)
    copies["chan"].wait()
    for name in ("wout", "square", "outer", "inner"):
        copies[name].start()

    def exchange(stage, half, tt):
        target = lax.rem(plane + plane_step(tt), 4)
        src, dst = send.at[stage, half], recv.at[stage, half]
        for step in STEPS:
            dx, dy, dc = step
            to_row, to_col = target * 4 + xs[dx], cols[dy][dc]

            def start():
                pltpu.make_async_remote_copy(
                    src.at[to_row * 8 + to_col], dst.at[me], ssem.at[stage, half], rsem.at[stage, half, plane],
                    device_id={"row": to_row, "col": to_col}, device_id_type=MESH,
                ).start()

            if step == (0, 0, 0):
                when(tt != PLANES - 1, start)
            else:
                start()

        def keep():
            recv[stage, half, me] = send[stage, half, me]

        when(tt == PLANES - 1, keep)

    def exchange_all(stage, half):
        src, dst = send.at[stage, half], recv.at[stage, half]
        for dz, dx, dy, dc in EVERY:
            to_row, to_col = planes[dz] * 4 + xs[dx], cols[dy][dc]
            pltpu.make_async_remote_copy(
                src.at[to_row * 8 + to_col], dst.at[me], ssem.at[stage, half], rsem.at[stage, half, plane],
                device_id={"row": to_row, "col": to_col}, device_id_type=MESH,
            ).start()
        recv[stage, half, me] = send[stage, half, me]

    def arrive(stage, half, tt):
        source = lax.rem(plane + 4 - plane_step(tt), 4)

        def wait(count):
            ref = recv.at[stage, half, pl.ds(0, count)]
            pltpu.make_async_remote_copy(
                ref, ref, ssem.at[stage, half], rsem.at[stage, half, source],
                device_id={"row": row, "col": col}, device_id_type=MESH,
            ).wait_recv()

        when(tt != PLANES - 1, lambda: wait(PER))
        when(tt == PLANES - 1, lambda: wait(PER - 1))
        return source

    def block_of(stage, half, source):
        return recv[stage, half, pl.ds(source * PER, PER)].reshape(256, HALF)

    def channels(half, tt):
        target = lax.rem(plane + plane_step(tt), 4)
        rows = pl.ds(half * 256, 256)
        v = sum(
            lax.dot_general(
                chan[part, j, rows], hs[tt, j * HALF : j * HALF + HALF], LAST, preferred_element_type=F32
            )
            for j in range(2)
            for part in range(2)
        )
        send[0, half, pl.ds(target * PER, PER)] = v.reshape(PER, 8, HALF).astype(BF16)

    channels(0, 0)
    pl.semaphore_wait(barrier, 127)
    exchange(0, 0, 0)

    @pl.loop(1, PLANES)
    def _(tt):
        win_copy(tt).wait()
        hs[tt] = jnp.dot(tok[...], win[tt], preferred_element_type=F32).astype(BF16)
        channels(0, tt)
        exchange(0, 0, tt)

    @pl.loop(0, PLANES)
    def _(tt):
        channels(1, tt)
        exchange(0, 1, tt)


    @pl.loop(0, 8)
    def _(i):
        rows = pl.ds(pl.multiple_of(i * 16, 16), 16)
        q = lax.broadcasted_iota(jnp.int32, (16, ROWS), 0) + i * 16
        j = lax.broadcasted_iota(jnp.int32, (16, ROWS), 1)
        turns = (q * j).astype(F32) * (1.0 / 65536) - 0.5
        square_turns = turns * turns
        twist[0, rows, :] = -polynomial(square_turns, series(0, 11))
        twist[1, rows, :] = -polynomial(square_turns, series(1, 11)) * turns

    for name in ("square", "outer", "inner"):
        copies[name].wait()

    special = lax.rem(me, 8) == 0
    @pl.loop(0, 2)
    def _(half):
        alike = jnp.logical_and(special, half == 0)

        @pl.loop(0, PLANES)
        def _(tt):
            source = arrive(0, half, tt)
            v = jnp.dot(square[0], block_of(0, half, source), preferred_element_type=F32).astype(BF16)
            for h in range(2):
                for slot in range(4):
                    xb[slot, pl.ds(pl.multiple_of(source * PER, PER), PER), h * HALF : h * HALF + HALF] = v[
                        (h * 4 + slot) * PER : (h * 4 + slot + 1) * PER
                    ]

        for cp in range(2):
            parts = []
            for slot in (2 * cp, 2 * cp + 1):
                a = jnp.dot(
                    outer[...], jnp.concatenate([xb[slot], xb[slot]], axis=0), preferred_element_type=F32
                )
                re, im = a[:128], a[128:]
                b_re = re * twist[0] + im * twist[1]
                b_im = im * twist[0] - re * twist[1]
                if slot == 2:
                    b_re, b_im = jnp.where(alike, b_re, -b_im), jnp.where(alike, b_im, b_re)
                elif slot >= 2:
                    b_re, b_im = -b_im, b_re
                parts.append(jnp.concatenate([b_re.astype(BF16), b_im.astype(BF16)], axis=1))
            b = jnp.concatenate(parts, axis=0)
            t = lax.dot_general(inner[...], b, LAST, preferred_element_type=F32)
            for eb in range(4):
                for s in range(4):
                    for c in range(2):
                        place = (s // 2) * 4 + 2 * cp + c
                        ts[eb, place * PER : place * PER + PER, s % 2 * 128 : s % 2 * 128 + 128] = t[
                            (eb * 4 + s) * PER : (eb * 4 + s + 1) * PER, c * 128 : c * 128 + 128
                        ].astype(BF16)

        for z in range(PLANES):
            v = jnp.dot(square[1], ts[z], preferred_element_type=F32)
            send[1, half, z * PER : z * PER + PER] = v.reshape(PER, 8, HALF).astype(BF16)
        for tt in range(PLANES):
            exchange(1, half, tt)

    copies["wout"].wait()

    @pl.loop(0, PLANES)
    def _(z):
        rows = pl.ds(pl.multiple_of(z * 256, 256), 256)
        half_rows = pl.ds(pl.multiple_of(z * 128, 128), 128)

        @pl.loop(0, 1)
        def _(n):
            columns = pl.ds(pl.multiple_of(n * 4096, 4096), 4096)
            w = jnp.dot(square[2], wout[rows, columns], preferred_element_type=F32).astype(BF16)
            wmix_a[half_rows, columns] = w[:128]
            wmix_b[half_rows, columns] = w[128:]

    for half, spec in enumerate((spec_a, spec_b)):
        for tt in range(PLANES):
            arrive(1, half, tt)
        for z in range(PLANES):
            v = lax.dot_general(block_of(1, half, z), square[1], FIRST, preferred_element_type=F32).astype(BF16)
            spec[:HALF, z * 128 : z * 128 + 128] = v[:, :128]
            spec[HALF:, z * 128 : z * 128 + 128] = v[:, 128:]

        if half == 0:
            @pl.loop(0, 4)
            def _(n):
                columns = pl.ds(pl.multiple_of(n * 1024, 1024), 1024)
                acc[:, columns] = jnp.dot(spec_a[...], wmix_a[:, columns], preferred_element_type=F32)

    for stage in range(2):
        for half in range(2):
            ref = send.at[stage, half, pl.ds(0, 127)]
            pltpu.make_async_remote_copy(
                ref, ref, ssem.at[stage, half], rsem.at[stage, half, 0],
                device_id={"row": row, "col": col}, device_id_type=MESH,
            ).wait_send()


def finish(acc, spec_b, wmix_b, out_hbm, buf, sem):
    copies = []
    for n in range(8):
        columns = pl.ds(n * 512, 512)
        v = jnp.dot(spec_b[...], wmix_b[:, columns], preferred_element_type=F32)
        buf[n] = (acc[:, columns] + v).astype(BF16)
        copies.append(pltpu.make_async_copy(buf.at[n], out_hbm.at[:, columns], sem.at[n]))
        copies[n].start()
    for copy in copies:
        copy.wait()


def local(tokens, norm_gain, in_weight, out_weight):
    constants = [pltpu.with_memory_space_constraint(jnp.asarray(t), pltpu.HBM) for t in tables()]
    tokens, norm_gain, in_weight, out_weight = (
        pltpu.with_memory_space_constraint(a, pltpu.HBM) for a in (tokens, norm_gain, in_weight, out_weight)
    )
    hbm = pl.BlockSpec(memory_space=pltpu.HBM)
    vmem = pl.BlockSpec(memory_space=pltpu.VMEM)
    acc, spec_b, wmix_b = pl.pallas_call(
        mixer,
        out_shape=[
            jax.ShapeDtypeStruct((ROWS, WIDTH), F32),
            jax.ShapeDtypeStruct((ROWS, 512), BF16),
            jax.ShapeDtypeStruct((512, WIDTH), BF16),
        ],
        in_specs=[hbm] * 8,
        out_specs=[vmem] * 3,
        scratch_shapes=[
            pltpu.VMEM((ROWS, WIDTH), BF16),
            pltpu.VMEM((WIDTH,), BF16),
            pltpu.VMEM((PLANES, WIDTH, 256), BF16),
            pltpu.VMEM((1024, WIDTH), BF16),
            pltpu.VMEM((512, WIDTH), BF16),
            pltpu.VMEM((2, 2, 512, 256), BF16),
            pltpu.VMEM((3, 256, 256), BF16),
            pltpu.VMEM((256, 256), BF16),
            pltpu.VMEM((2, 128, 512), F32),
            pltpu.VMEM((512, 1024), BF16),
            pltpu.VMEM((PLANES, ROWS, 256), BF16),
            pltpu.VMEM((2, 2, 128, 8, HALF), BF16),
            pltpu.VMEM((2, 2, 128, 8, HALF), BF16),
            pltpu.VMEM((4, 128, 512), BF16),
            pltpu.VMEM((4, 256, HALF), BF16),
            pltpu.VMEM((ROWS, 512), BF16),
            pltpu.SemaphoreType.DMA((8,)),
            pltpu.SemaphoreType.DMA((4,)),
            pltpu.SemaphoreType.DMA((7,)),
            pltpu.SemaphoreType.DMA((2, 2)),
            pltpu.SemaphoreType.DMA((2, 2, 4)),
        ],
        compiler_params=pltpu.CompilerParams(
            collective_id=0, has_side_effects=True, vmem_limit_bytes=MIXER_VMEM
        ),
        name="mixer",
    )(tokens, norm_gain, in_weight, out_weight, *constants)
    return pl.pallas_call(
        finish,
        out_shape=jax.ShapeDtypeStruct((ROWS, WIDTH), BF16),
        in_specs=[vmem] * 3,
        out_specs=hbm,
        scratch_shapes=[pltpu.VMEM((8, ROWS, 512), BF16), pltpu.SemaphoreType.DMA((8,))],
        compiler_params=pltpu.CompilerParams(vmem_limit_bytes=FINISH_VMEM),
        name="finish",
    )(acc, spec_b, wmix_b)


MIXER_VMEM = 40 * 2**20
FINISH_VMEM = 8 * 2**20


def solution(mesh):
    placed = (P(("row", "col"), None), P(), P(), P())
    return jax.shard_map(
        local, mesh=mesh, in_specs=placed, out_specs=P(("row", "col"), None), check_vma=False
    )
```

```python
import math
import random

import jax
import jax.numpy as jnp
import numpy as np
from jax import lax
from jax.experimental import pallas as pl
from jax.experimental.pallas import tpu as pltpu
from jax.sharding import PartitionSpec as P

ROWS = 512
WIDTH = 4096
PLANES = 4
PER = 32
HALF = 256
MESH = pl.DeviceIdType.MESH
F32 = jnp.float32
BF16 = jnp.bfloat16
LAST = (((1,), (1,)), ((), ()))
FIRST = (((0,), (0,)), ((), ()))


def slot_pair(half, i, slot):
    return 4 * i + 2 * half + slot % 2


def channel_table():
    table = np.zeros((2, 2, 4, 8, 2, 4, 256))
    c = np.arange(64)
    for half in range(2):
        for g in range(4):
            for i in range(8):
                for slot in range(4):
                    p = slot_pair(half, i, slot)
                    if slot < 2:
                        row = np.cos(2 * np.pi * c * p / 64)
                    elif p == 0:
                        row = np.cos(np.pi * c)
                    else:
                        row = -np.sin(2 * np.pi * c * p / 64)
                    for h in range(2):
                        table[h, half, g, i, h, slot, g * 64 : g * 64 + 64] = row / 8
    return table.reshape(2, 512, 256)


def weight_table():
    table = np.zeros((2, 4, 4, 8, 4, 64))
    for half in range(2):
        for g in range(4):
            for i in range(8):
                for slot in range(4):
                    p = slot_pair(half, i, slot)
                    if p == 0:
                        table[half, slot, g, i, g, 0 if slot < 2 else 32] = 1
                    else:
                        table[half, slot, g, i, g, p] = 1
                        table[half, slot, g, i, g, 64 - p] = 1 if slot < 2 else -1
    return table.reshape(256, 256)


def swap_table():
    table = np.zeros((256, 256))
    for d in range(PER):
        for slot in range(8):
            table[slot * PER + d, d * 8 + slot] = 1
    return table


def tables():
    chan = channel_table()
    high = chan.astype(BF16)
    low = (chan - high.astype(np.float64)).astype(BF16)
    chan = np.stack([high, low])
    swap = swap_table()
    square = np.stack([swap, swap.T, weight_table()]).astype(BF16)
    d = np.arange(128)
    angle = 2 * np.pi * ((d[:, None] * d[None, :]) % 128) / 128
    outer = np.concatenate([np.cos(angle), -np.sin(angle)])
    outer_high = outer.astype(BF16)
    outer = np.concatenate([outer_high, (outer - outer_high.astype(np.float64)).astype(BF16)], axis=1)
    j = np.arange(512)
    e = np.arange(128).reshape(4, 1, 32)
    s = np.arange(4).reshape(1, 4, 1)
    p = (4 * e + s).reshape(512)
    angle = 2 * np.pi * ((p[:, None] * j[None, :]) % 512) / 512
    inner = (np.concatenate([np.cos(angle), np.sin(angle)], axis=1) / 256).astype(BF16)
    return chan, square, outer, inner


def series(first, count):
    return [
        (-1) ** k * (2 * math.pi) ** (2 * k + first) / math.factorial(2 * k + first) for k in range(count)
    ]


def polynomial(t, coefficients):
    total = jnp.full_like(t, coefficients[-1])
    for c in coefficients[-2::-1]:
        total = total * t + c
    return total


def hops(*steps):
    return sum(min(s, 4 - s) for s in steps)


EVERY = [
    (a, b, c, d) for a in range(4) for b in range(4) for c in range(4) for d in range(2) if (a, b, c, d) != (0, 0, 0, 0)
]
random.Random(2).shuffle(EVERY)
EVERY.sort(key=lambda s: -hops(*s[:3]))
STEPS = [(b, c, d) for b in range(4) for c in range(4) for d in range(2) if (b, c, d) != (0, 0, 0)]
random.Random(3).shuffle(STEPS)
STEPS.sort(key=lambda s: -hops(*s[:2]))
STEPS.append((0, 0, 0))


def when(condition, action):
    if isinstance(condition, bool):
        if condition:
            action()
    else:
        pl.when(condition)(action)


def plane_step(tt):
    steps = (1, 2, 3, 0)
    if isinstance(tt, int):
        return steps[tt]
    return sum(jnp.where(tt == i, step, 0) for i, step in enumerate(steps))


def mixer(
    tok_hbm, gain_hbm, win_hbm, wout_hbm, chan_hbm, square_hbm, outer_hbm, inner_hbm,
    acc, spec_b, wmix_b,
    tok, gain_ref, win, wout, wmix_a, chan, square, outer, twist, inner,
    hs, send, recv, xb, ts, spec_a,
    tok_sem, win_sem, tab_sem, ssem, rsem,
):
    row, col = lax.axis_index("row"), lax.axis_index("col")
    me = row * 8 + col
    plane, x = lax.div(row, 4), lax.rem(row, 4)
    y, core = lax.div(col, 2), lax.rem(col, 2)
    planes = [lax.rem(plane + i, 4) for i in range(4)]
    xs = [lax.rem(x + i, 4) for i in range(4)]
    cols = [[lax.rem(y + i, 4) * 2 + (core if c == 0 else 1 - core) for c in range(2)] for i in range(4)]

    gain_copy = pltpu.make_async_copy(gain_hbm, gain_ref, tab_sem.at[0])
    gain_copy.start()
    tok_copies = []
    for i in range(8):
        rows = pl.ds(i * 64, 64)
        copy = pltpu.make_async_copy(tok_hbm.at[rows], tok.at[rows], tok_sem.at[i])
        tok_copies.append(copy)

    def win_copy(tt):
        target = lax.rem(plane + plane_step(tt), 4)
        columns = pl.ds(pl.multiple_of(target * 256, 256), 256)
        return pltpu.make_async_copy(win_hbm.at[:, columns], win.at[tt], win_sem.at[tt])

    copies = {}
    for i, (name, a, b) in enumerate(
        (
            ("chan", chan_hbm, chan), ("square", square_hbm, square), ("outer", outer_hbm, outer),
            ("inner", inner_hbm, inner), ("wout", wout_hbm, wout),
        )
    ):
        copies[name] = pltpu.make_async_copy(a, b, tab_sem.at[i + 1])
    for i in range(3):
        tok_copies[i].start()
    win_copy(0).start()
    for i in range(3, 8):
        tok_copies[i].start()
    barrier = pltpu.get_barrier_semaphore()

    @pl.loop(0, 16)
    def _(d):
        to_row = lax.rem(plane + 2 + lax.div(d, 4), 4) * 4 + lax.rem(x + d, 4)
        for dy in range(4):
            for dc in range(2):
                to_col = cols[dy][dc]

                def signal():
                    pl.semaphore_signal(barrier, 1, device_id={"row": to_row, "col": to_col}, device_id_type=MESH)

                if dy == 0 and dc == 0:
                    pl.when(to_row != row)(signal)
                else:
                    signal()

    gain_copy.wait()
    gain = gain_ref[...].astype(F32).reshape(1, WIDTH)

    for i in range(8):
        tok_copies[i].wait()
        rows = slice(i * 64, i * 64 + 64)
        v = tok[rows, :].astype(F32)
        scale = lax.rsqrt(jnp.mean(v * v, axis=-1, keepdims=True) + 1e-06)
        tok[rows, :] = (v * scale * gain).astype(BF16)
        if i == 1:
            copies["chan"].start()
            win_copy(1).start()
        if i == 3:
            win_copy(2).start()
            win_copy(3).start()
    win_copy(0).wait()
    hs[0] = jnp.dot(tok[...], win[0], preferred_element_type=F32).astype(BF16)
    copies["chan"].wait()
    for name in ("wout", "square", "outer", "inner"):
        copies[name].start()

    def exchange(stage, half, tt):
        target = lax.rem(plane + plane_step(tt), 4)
        src, dst = send.at[stage, half], recv.at[stage, half]
        for step in STEPS:
            dx, dy, dc = step
            to_row, to_col = target * 4 + xs[dx], cols[dy][dc]

            def start():
                pltpu.make_async_remote_copy(
                    src.at[to_row * 8 + to_col], dst.at[me], ssem.at[stage, half], rsem.at[stage, half, plane],
                    device_id={"row": to_row, "col": to_col}, device_id_type=MESH,
                ).start()

            if step == (0, 0, 0):
                when(tt != PLANES - 1, start)
            else:
                start()

        def keep():
            recv[stage, half, me] = send[stage, half, me]

        when(tt == PLANES - 1, keep)

    def exchange_all(stage, half):
        src, dst = send.at[stage, half], recv.at[stage, half]
        for dz, dx, dy, dc in EVERY:
            to_row, to_col = planes[dz] * 4 + xs[dx], cols[dy][dc]
            pltpu.make_async_remote_copy(
                src.at[to_row * 8 + to_col], dst.at[me], ssem.at[stage, half], rsem.at[stage, half, plane],
                device_id={"row": to_row, "col": to_col}, device_id_type=MESH,
            ).start()
        recv[stage, half, me] = send[stage, half, me]

    def arrive(stage, half, tt):
        source = lax.rem(plane + 4 - plane_step(tt), 4)

        def wait(count):
            ref = recv.at[stage, half, pl.ds(0, count)]
            pltpu.make_async_remote_copy(
                ref, ref, ssem.at[stage, half], rsem.at[stage, half, source],
                device_id={"row": row, "col": col}, device_id_type=MESH,
            ).wait_recv()

        when(tt != PLANES - 1, lambda: wait(PER))
        when(tt == PLANES - 1, lambda: wait(PER - 1))
        return source

    def block_of(stage, half, source):
        return recv[stage, half, pl.ds(source * PER, PER)].reshape(256, HALF)

    def channels(half, tt):
        target = lax.rem(plane + plane_step(tt), 4)
        rows = pl.ds(half * 256, 256)
        v = sum(
            lax.dot_general(
                chan[part, j, rows], hs[tt, j * HALF : j * HALF + HALF], LAST, preferred_element_type=F32
            )
            for j in range(2)
            for part in range(2)
        )
        send[0, half, pl.ds(target * PER, PER)] = v.reshape(PER, 8, HALF).astype(BF16)

    channels(0, 0)
    pl.semaphore_wait(barrier, 127)
    exchange(0, 0, 0)

    @pl.loop(1, PLANES)
    def _(tt):
        win_copy(tt).wait()
        hs[tt] = jnp.dot(tok[...], win[tt], preferred_element_type=F32).astype(BF16)
        channels(0, tt)
        exchange(0, 0, tt)

    @pl.loop(0, PLANES)
    def _(tt):
        channels(1, tt)
        exchange(0, 1, tt)


    @pl.loop(0, 8)
    def _(i):
        rows = pl.ds(pl.multiple_of(i * 16, 16), 16)
        q = lax.broadcasted_iota(jnp.int32, (16, ROWS), 0) + i * 16
        j = lax.broadcasted_iota(jnp.int32, (16, ROWS), 1)
        turns = (q * j).astype(F32) * (1.0 / 65536) - 0.5
        square_turns = turns * turns
        twist[0, rows, :] = -polynomial(square_turns, series(0, 11))
        twist[1, rows, :] = -polynomial(square_turns, series(1, 11)) * turns

    for name in ("square", "outer", "inner"):
        copies[name].wait()

    special = lax.rem(me, 8) == 0
    @pl.loop(0, 2)
    def _(half):
        alike = jnp.logical_and(special, half == 0)

        @pl.loop(0, PLANES)
        def _(tt):
            source = arrive(0, half, tt)
            v = jnp.dot(square[0], block_of(0, half, source), preferred_element_type=F32).astype(BF16)
            for h in range(2):
                for slot in range(4):
                    xb[slot, pl.ds(pl.multiple_of(source * PER, PER), PER), h * HALF : h * HALF + HALF] = v[
                        (h * 4 + slot) * PER : (h * 4 + slot + 1) * PER
                    ]

        for cp in range(2):
            parts = []
            for slot in (2 * cp, 2 * cp + 1):
                a = jnp.dot(
                    outer[...], jnp.concatenate([xb[slot], xb[slot]], axis=0), preferred_element_type=F32
                )
                re, im = a[:128], a[128:]
                b_re = re * twist[0] + im * twist[1]
                b_im = im * twist[0] - re * twist[1]
                if slot == 2:
                    b_re, b_im = jnp.where(alike, b_re, -b_im), jnp.where(alike, b_im, b_re)
                elif slot >= 2:
                    b_re, b_im = -b_im, b_re
                parts.append(jnp.concatenate([b_re.astype(BF16), b_im.astype(BF16)], axis=1))
            b = jnp.concatenate(parts, axis=0)
            t = lax.dot_general(inner[...], b, LAST, preferred_element_type=F32)
            for eb in range(4):
                for s in range(4):
                    for c in range(2):
                        place = (s // 2) * 4 + 2 * cp + c
                        ts[eb, place * PER : place * PER + PER, s % 2 * 128 : s % 2 * 128 + 128] = t[
                            (eb * 4 + s) * PER : (eb * 4 + s + 1) * PER, c * 128 : c * 128 + 128
                        ].astype(BF16)

        for z in range(PLANES):
            v = jnp.dot(square[1], ts[z], preferred_element_type=F32)
            send[1, half, z * PER : z * PER + PER] = v.reshape(PER, 8, HALF).astype(BF16)
        for tt in range(PLANES):
            exchange(1, half, tt)

    copies["wout"].wait()

    @pl.loop(0, PLANES)
    def _(z):
        rows = pl.ds(pl.multiple_of(z * 256, 256), 256)
        half_rows = pl.ds(pl.multiple_of(z * 128, 128), 128)

        @pl.loop(0, 1)
        def _(n):
            columns = pl.ds(pl.multiple_of(n * 4096, 4096), 4096)
            w = jnp.dot(square[2], wout[rows, columns], preferred_element_type=F32).astype(BF16)
            wmix_a[half_rows, columns] = w[:128]
            wmix_b[half_rows, columns] = w[128:]

    for half, spec in enumerate((spec_a, spec_b)):
        for tt in range(PLANES):
            arrive(1, half, tt)
        for z in range(PLANES):
            v = lax.dot_general(block_of(1, half, z), square[1], FIRST, preferred_element_type=F32).astype(BF16)
            spec[:HALF, z * 128 : z * 128 + 128] = v[:, :128]
            spec[HALF:, z * 128 : z * 128 + 128] = v[:, 128:]

        if half == 0:
            @pl.loop(0, 2)
            def _(n):
                columns = pl.ds(pl.multiple_of(n * 2048, 2048), 2048)
                acc[:, columns] = jnp.dot(spec_a[...], wmix_a[:, columns], preferred_element_type=F32)

    for stage in range(2):
        for half in range(2):
            ref = send.at[stage, half, pl.ds(0, 127)]
            pltpu.make_async_remote_copy(
                ref, ref, ssem.at[stage, half], rsem.at[stage, half, 0],
                device_id={"row": row, "col": col}, device_id_type=MESH,
            ).wait_send()


def finish(acc, spec_b, wmix_b, out_hbm, buf, sem):
    copies = []
    for n in range(8):
        columns = pl.ds(n * 512, 512)
        v = jnp.dot(spec_b[...], wmix_b[:, columns], preferred_element_type=F32)
        buf[n] = (acc[:, columns] + v).astype(BF16)
        copies.append(pltpu.make_async_copy(buf.at[n], out_hbm.at[:, columns], sem.at[n]))
        copies[n].start()
    for copy in copies:
        copy.wait()


def local(tokens, norm_gain, in_weight, out_weight):
    constants = [pltpu.with_memory_space_constraint(jnp.asarray(t), pltpu.HBM) for t in tables()]
    tokens, norm_gain, in_weight, out_weight = (
        pltpu.with_memory_space_constraint(a, pltpu.HBM) for a in (tokens, norm_gain, in_weight, out_weight)
    )
    hbm = pl.BlockSpec(memory_space=pltpu.HBM)
    vmem = pl.BlockSpec(memory_space=pltpu.VMEM)
    acc, spec_b, wmix_b = pl.pallas_call(
        mixer,
        out_shape=[
            jax.ShapeDtypeStruct((ROWS, WIDTH), F32),
            jax.ShapeDtypeStruct((ROWS, 512), BF16),
            jax.ShapeDtypeStruct((512, WIDTH), BF16),
        ],
        in_specs=[hbm] * 8,
        out_specs=[vmem] * 3,
        scratch_shapes=[
            pltpu.VMEM((ROWS, WIDTH), BF16),
            pltpu.VMEM((WIDTH,), BF16),
            pltpu.VMEM((PLANES, WIDTH, 256), BF16),
            pltpu.VMEM((1024, WIDTH), BF16),
            pltpu.VMEM((512, WIDTH), BF16),
            pltpu.VMEM((2, 2, 512, 256), BF16),
            pltpu.VMEM((3, 256, 256), BF16),
            pltpu.VMEM((256, 256), BF16),
            pltpu.VMEM((2, 128, 512), F32),
            pltpu.VMEM((512, 1024), BF16),
            pltpu.VMEM((PLANES, ROWS, 256), BF16),
            pltpu.VMEM((2, 2, 128, 8, HALF), BF16),
            pltpu.VMEM((2, 2, 128, 8, HALF), BF16),
            pltpu.VMEM((4, 128, 512), BF16),
            pltpu.VMEM((4, 256, HALF), BF16),
            pltpu.VMEM((ROWS, 512), BF16),
            pltpu.SemaphoreType.DMA((8,)),
            pltpu.SemaphoreType.DMA((4,)),
            pltpu.SemaphoreType.DMA((7,)),
            pltpu.SemaphoreType.DMA((2, 2)),
            pltpu.SemaphoreType.DMA((2, 2, 4)),
        ],
        compiler_params=pltpu.CompilerParams(
            collective_id=0, has_side_effects=True, vmem_limit_bytes=MIXER_VMEM
        ),
        name="mixer",
    )(tokens, norm_gain, in_weight, out_weight, *constants)
    return pl.pallas_call(
        finish,
        out_shape=jax.ShapeDtypeStruct((ROWS, WIDTH), BF16),
        in_specs=[vmem] * 3,
        out_specs=hbm,
        scratch_shapes=[pltpu.VMEM((8, ROWS, 512), BF16), pltpu.SemaphoreType.DMA((8,))],
        compiler_params=pltpu.CompilerParams(vmem_limit_bytes=FINISH_VMEM),
        name="finish",
    )(acc, spec_b, wmix_b)


MIXER_VMEM = 40 * 2**20
FINISH_VMEM = 8 * 2**20


def solution(mesh):
    placed = (P(("row", "col"), None), P(), P(), P())
    return jax.shard_map(
        local, mesh=mesh, in_specs=placed, out_specs=P(("row", "col"), None), check_vma=False
    )
```

```python
import math
import random

import jax
import jax.numpy as jnp
import numpy as np
from jax import lax
from jax.experimental import pallas as pl
from jax.experimental.pallas import tpu as pltpu
from jax.sharding import PartitionSpec as P

ROWS = 512
WIDTH = 4096
PLANES = 4
PER = 32
HALF = 256
MESH = pl.DeviceIdType.MESH
F32 = jnp.float32
BF16 = jnp.bfloat16
LAST = (((1,), (1,)), ((), ()))
FIRST = (((0,), (0,)), ((), ()))


def slot_pair(half, i, slot):
    return 4 * i + 2 * half + slot % 2


def channel_table():
    table = np.zeros((2, 2, 4, 8, 2, 4, 256))
    c = np.arange(64)
    for half in range(2):
        for g in range(4):
            for i in range(8):
                for slot in range(4):
                    p = slot_pair(half, i, slot)
                    if slot < 2:
                        row = np.cos(2 * np.pi * c * p / 64)
                    elif p == 0:
                        row = np.cos(np.pi * c)
                    else:
                        row = -np.sin(2 * np.pi * c * p / 64)
                    for h in range(2):
                        table[h, half, g, i, h, slot, g * 64 : g * 64 + 64] = row / 8
    return table.reshape(2, 512, 256)


def weight_table():
    table = np.zeros((2, 4, 4, 8, 4, 64))
    for half in range(2):
        for g in range(4):
            for i in range(8):
                for slot in range(4):
                    p = slot_pair(half, i, slot)
                    if p == 0:
                        table[half, slot, g, i, g, 0 if slot < 2 else 32] = 1
                    else:
                        table[half, slot, g, i, g, p] = 1
                        table[half, slot, g, i, g, 64 - p] = 1 if slot < 2 else -1
    return table.reshape(256, 256)


def swap_table():
    table = np.zeros((256, 256))
    for d in range(PER):
        for slot in range(8):
            table[slot * PER + d, d * 8 + slot] = 1
    return table


def tables():
    chan = channel_table()
    high = chan.astype(BF16)
    low = (chan - high.astype(np.float64)).astype(BF16)
    chan = np.stack([high, low])
    swap = swap_table()
    square = np.stack([swap, swap.T, weight_table()]).astype(BF16)
    d = np.arange(128)
    angle = 2 * np.pi * ((d[:, None] * d[None, :]) % 128) / 128
    outer = np.concatenate([np.cos(angle), -np.sin(angle)]).astype(BF16)
    j = np.arange(512)
    e = np.arange(128).reshape(4, 1, 32)
    s = np.arange(4).reshape(1, 4, 1)
    p = (4 * e + s).reshape(512)
    angle = 2 * np.pi * ((p[:, None] * j[None, :]) % 512) / 512
    inner = (np.concatenate([np.cos(angle), np.sin(angle)], axis=1) / 256).astype(BF16)
    return chan, square, outer, inner


def series(first, count):
    return [
        (-1) ** k * (2 * math.pi) ** (2 * k + first) / math.factorial(2 * k + first) for k in range(count)
    ]


def polynomial(t, coefficients):
    total = jnp.full_like(t, coefficients[-1])
    for c in coefficients[-2::-1]:
        total = total * t + c
    return total


def hops(*steps):
    return sum(min(s, 4 - s) for s in steps)


EVERY = [
    (a, b, c, d) for a in range(4) for b in range(4) for c in range(4) for d in range(2) if (a, b, c, d) != (0, 0, 0, 0)
]
random.Random(2).shuffle(EVERY)
EVERY.sort(key=lambda s: -hops(*s[:3]))
STEPS = [(b, c, d) for b in range(4) for c in range(4) for d in range(2) if (b, c, d) != (0, 0, 0)]
random.Random(3).shuffle(STEPS)
STEPS.sort(key=lambda s: -hops(*s[:2]))
STEPS.append((0, 0, 0))


def when(condition, action):
    if isinstance(condition, bool):
        if condition:
            action()
    else:
        pl.when(condition)(action)


def plane_step(tt):
    steps = (1, 2, 3, 0)
    if isinstance(tt, int):
        return steps[tt]
    return sum(jnp.where(tt == i, step, 0) for i, step in enumerate(steps))


def mixer(
    tok_hbm, gain_hbm, win_hbm, wout_hbm, chan_hbm, square_hbm, outer_hbm, inner_hbm,
    acc, spec_b, wmix_b,
    tok, gain_ref, win, wout, wmix_a, chan, square, outer, twist, inner,
    hs, send, recv, xb, ts, spec_a,
    tok_sem, win_sem, tab_sem, ssem, rsem,
):
    row, col = lax.axis_index("row"), lax.axis_index("col")
    me = row * 8 + col
    plane, x = lax.div(row, 4), lax.rem(row, 4)
    y, core = lax.div(col, 2), lax.rem(col, 2)
    planes = [lax.rem(plane + i, 4) for i in range(4)]
    xs = [lax.rem(x + i, 4) for i in range(4)]
    cols = [[lax.rem(y + i, 4) * 2 + (core if c == 0 else 1 - core) for c in range(2)] for i in range(4)]

    gain_copy = pltpu.make_async_copy(gain_hbm, gain_ref, tab_sem.at[0])
    gain_copy.start()
    tok_copies = []
    for i in range(8):
        rows = pl.ds(i * 64, 64)
        copy = pltpu.make_async_copy(tok_hbm.at[rows], tok.at[rows], tok_sem.at[i])
        tok_copies.append(copy)

    def win_copy(tt):
        target = lax.rem(plane + plane_step(tt), 4)
        columns = pl.ds(pl.multiple_of(target * 256, 256), 256)
        return pltpu.make_async_copy(win_hbm.at[:, columns], win.at[tt], win_sem.at[tt])

    copies = {}
    for i, (name, a, b) in enumerate(
        (
            ("chan", chan_hbm, chan), ("square", square_hbm, square), ("outer", outer_hbm, outer),
            ("inner", inner_hbm, inner), ("wout", wout_hbm, wout),
        )
    ):
        copies[name] = pltpu.make_async_copy(a, b, tab_sem.at[i + 1])
    for i in range(3):
        tok_copies[i].start()
    win_copy(0).start()
    for i in range(3, 8):
        tok_copies[i].start()
    barrier = pltpu.get_barrier_semaphore()

    @pl.loop(0, 16)
    def _(d):
        to_row = lax.rem(plane + 2 + lax.div(d, 4), 4) * 4 + lax.rem(x + d, 4)
        for dy in range(4):
            for dc in range(2):
                to_col = cols[dy][dc]

                def signal():
                    pl.semaphore_signal(barrier, 1, device_id={"row": to_row, "col": to_col}, device_id_type=MESH)

                if dy == 0 and dc == 0:
                    pl.when(to_row != row)(signal)
                else:
                    signal()

    gain_copy.wait()
    gain = gain_ref[...].astype(F32).reshape(1, WIDTH)

    for i in range(8):
        tok_copies[i].wait()
        rows = slice(i * 64, i * 64 + 64)
        v = tok[rows, :].astype(F32)
        scale = lax.rsqrt(jnp.mean(v * v, axis=-1, keepdims=True) + 1e-06)
        tok[rows, :] = (v * scale * gain).astype(BF16)
        if i == 1:
            copies["chan"].start()
            win_copy(1).start()
        if i == 3:
            win_copy(2).start()
            win_copy(3).start()
    win_copy(0).wait()
    hs[0] = jnp.dot(tok[...], win[0], preferred_element_type=F32).astype(BF16)
    copies["chan"].wait()
    for name in ("wout", "square", "outer", "inner"):
        copies[name].start()

    def exchange(stage, half, tt):
        target = lax.rem(plane + plane_step(tt), 4)
        src, dst = send.at[stage, half], recv.at[stage, half]
        for step in STEPS:
            dx, dy, dc = step
            to_row, to_col = target * 4 + xs[dx], cols[dy][dc]

            def start():
                pltpu.make_async_remote_copy(
                    src.at[to_row * 8 + to_col], dst.at[me], ssem.at[stage, half], rsem.at[stage, half, plane],
                    device_id={"row": to_row, "col": to_col}, device_id_type=MESH,
                ).start()

            if step == (0, 0, 0):
                when(tt != PLANES - 1, start)
            else:
                start()

        def keep():
            recv[stage, half, me] = send[stage, half, me]

        when(tt == PLANES - 1, keep)

    def exchange_all(stage, half):
        src, dst = send.at[stage, half], recv.at[stage, half]
        for dz, dx, dy, dc in EVERY:
            to_row, to_col = planes[dz] * 4 + xs[dx], cols[dy][dc]
            pltpu.make_async_remote_copy(
                src.at[to_row * 8 + to_col], dst.at[me], ssem.at[stage, half], rsem.at[stage, half, plane],
                device_id={"row": to_row, "col": to_col}, device_id_type=MESH,
            ).start()
        recv[stage, half, me] = send[stage, half, me]

    def arrive(stage, half, tt):
        source = lax.rem(plane + 4 - plane_step(tt), 4)

        def wait(count):
            ref = recv.at[stage, half, pl.ds(0, count)]
            pltpu.make_async_remote_copy(
                ref, ref, ssem.at[stage, half], rsem.at[stage, half, source],
                device_id={"row": row, "col": col}, device_id_type=MESH,
            ).wait_recv()

        when(tt != PLANES - 1, lambda: wait(PER))
        when(tt == PLANES - 1, lambda: wait(PER - 1))
        return source

    def block_of(stage, half, source):
        return recv[stage, half, pl.ds(source * PER, PER)].reshape(256, HALF)

    def channels(half, tt):
        target = lax.rem(plane + plane_step(tt), 4)
        rows = pl.ds(half * 256, 256)
        v = sum(
            lax.dot_general(
                chan[part, j, rows], hs[tt, j * HALF : j * HALF + HALF], LAST, preferred_element_type=F32
            )
            for j in range(2)
            for part in range(2)
        )
        send[0, half, pl.ds(target * PER, PER)] = v.reshape(PER, 8, HALF).astype(BF16)

    channels(0, 0)
    pl.semaphore_wait(barrier, 127)
    exchange(0, 0, 0)

    @pl.loop(1, PLANES)
    def _(tt):
        win_copy(tt).wait()
        hs[tt] = jnp.dot(tok[...], win[tt], preferred_element_type=F32).astype(BF16)
        channels(0, tt)
        exchange(0, 0, tt)

    @pl.loop(0, PLANES)
    def _(tt):
        channels(1, tt)
        exchange(0, 1, tt)


    @pl.loop(0, 8)
    def _(i):
        rows = pl.ds(pl.multiple_of(i * 16, 16), 16)
        q = lax.broadcasted_iota(jnp.int32, (16, ROWS), 0) + i * 16
        j = lax.broadcasted_iota(jnp.int32, (16, ROWS), 1)
        turns = (q * j).astype(F32) * (1.0 / 65536) - 0.5
        square_turns = turns * turns
        twist[0, rows, :] = -polynomial(square_turns, series(0, 11))
        twist[1, rows, :] = -polynomial(square_turns, series(1, 11)) * turns

    for name in ("square", "outer", "inner"):
        copies[name].wait()

    special = lax.rem(me, 8) == 0
    @pl.loop(0, 2)
    def _(half):
        alike = jnp.logical_and(special, half == 0)

        @pl.loop(0, PLANES)
        def _(tt):
            source = arrive(0, half, tt)
            v = jnp.dot(square[0], block_of(0, half, source), preferred_element_type=F32).astype(BF16)
            for h in range(2):
                for slot in range(4):
                    xb[slot, pl.ds(pl.multiple_of(source * PER, PER), PER), h * HALF : h * HALF + HALF] = v[
                        (h * 4 + slot) * PER : (h * 4 + slot + 1) * PER
                    ]

        for cp in range(2):
            parts = []
            for slot in (2 * cp, 2 * cp + 1):
                a = jnp.dot(outer[...], xb[slot], preferred_element_type=F32)
                re, im = a[:128], a[128:]
                b_re = re * twist[0] + im * twist[1]
                b_im = im * twist[0] - re * twist[1]
                if slot == 2:
                    b_re, b_im = jnp.where(alike, b_re, -b_im), jnp.where(alike, b_im, b_re)
                elif slot >= 2:
                    b_re, b_im = -b_im, b_re
                parts.append(jnp.concatenate([b_re.astype(BF16), b_im.astype(BF16)], axis=1))
            b = jnp.concatenate(parts, axis=0)
            t = lax.dot_general(inner[...], b, LAST, preferred_element_type=F32)
            for eb in range(4):
                for s in range(4):
                    for c in range(2):
                        place = (s // 2) * 4 + 2 * cp + c
                        ts[eb, place * PER : place * PER + PER, s % 2 * 128 : s % 2 * 128 + 128] = t[
                            (eb * 4 + s) * PER : (eb * 4 + s + 1) * PER, c * 128 : c * 128 + 128
                        ].astype(BF16)

        for z in range(PLANES):
            v = jnp.dot(square[1], ts[z], preferred_element_type=F32)
            send[1, half, z * PER : z * PER + PER] = v.reshape(PER, 8, HALF).astype(BF16)
        for tt in range(PLANES):
            exchange(1, half, tt)

    copies["wout"].wait()

    @pl.loop(0, PLANES)
    def _(z):
        rows = pl.ds(pl.multiple_of(z * 256, 256), 256)
        half_rows = pl.ds(pl.multiple_of(z * 128, 128), 128)

        @pl.loop(0, 1)
        def _(n):
            columns = pl.ds(pl.multiple_of(n * 4096, 4096), 4096)
            w = jnp.dot(square[2], wout[rows, columns], preferred_element_type=F32).astype(BF16)
            wmix_a[half_rows, columns] = w[:128]
            wmix_b[half_rows, columns] = w[128:]

    for half, spec in enumerate((spec_a, spec_b)):
        for tt in range(PLANES):
            arrive(1, half, tt)
        for z in range(PLANES):
            v = lax.dot_general(block_of(1, half, z), square[1], FIRST, preferred_element_type=F32).astype(BF16)
            spec[:HALF, z * 128 : z * 128 + 128] = v[:, :128]
            spec[HALF:, z * 128 : z * 128 + 128] = v[:, 128:]

        if half == 0:
            @pl.loop(0, 2)
            def _(n):
                columns = pl.ds(pl.multiple_of(n * 2048, 2048), 2048)
                acc[:, columns] = jnp.dot(spec_a[...], wmix_a[:, columns], preferred_element_type=F32)

    for stage in range(2):
        for half in range(2):
            ref = send.at[stage, half, pl.ds(0, 127)]
            pltpu.make_async_remote_copy(
                ref, ref, ssem.at[stage, half], rsem.at[stage, half, 0],
                device_id={"row": row, "col": col}, device_id_type=MESH,
            ).wait_send()


def finish(acc, spec_b, wmix_b, out_hbm, buf, sem):
    copies = []
    for n in range(8):
        columns = pl.ds(n * 512, 512)
        v = jnp.dot(spec_b[...], wmix_b[:, columns], preferred_element_type=F32)
        buf[n] = (acc[:, columns] + v).astype(BF16)
        copies.append(pltpu.make_async_copy(buf.at[n], out_hbm.at[:, columns], sem.at[n]))
        copies[n].start()
    for copy in copies:
        copy.wait()


def local(tokens, norm_gain, in_weight, out_weight):
    constants = [pltpu.with_memory_space_constraint(jnp.asarray(t), pltpu.HBM) for t in tables()]
    tokens, norm_gain, in_weight, out_weight = (
        pltpu.with_memory_space_constraint(a, pltpu.HBM) for a in (tokens, norm_gain, in_weight, out_weight)
    )
    hbm = pl.BlockSpec(memory_space=pltpu.HBM)
    vmem = pl.BlockSpec(memory_space=pltpu.VMEM)
    acc, spec_b, wmix_b = pl.pallas_call(
        mixer,
        out_shape=[
            jax.ShapeDtypeStruct((ROWS, WIDTH), F32),
            jax.ShapeDtypeStruct((ROWS, 512), BF16),
            jax.ShapeDtypeStruct((512, WIDTH), BF16),
        ],
        in_specs=[hbm] * 8,
        out_specs=[vmem] * 3,
        scratch_shapes=[
            pltpu.VMEM((ROWS, WIDTH), BF16),
            pltpu.VMEM((WIDTH,), BF16),
            pltpu.VMEM((PLANES, WIDTH, 256), BF16),
            pltpu.VMEM((1024, WIDTH), BF16),
            pltpu.VMEM((512, WIDTH), BF16),
            pltpu.VMEM((2, 2, 512, 256), BF16),
            pltpu.VMEM((3, 256, 256), BF16),
            pltpu.VMEM((256, 128), BF16),
            pltpu.VMEM((2, 128, 512), F32),
            pltpu.VMEM((512, 1024), BF16),
            pltpu.VMEM((PLANES, ROWS, 256), BF16),
            pltpu.VMEM((2, 2, 128, 8, HALF), BF16),
            pltpu.VMEM((2, 2, 128, 8, HALF), BF16),
            pltpu.VMEM((4, 128, 512), BF16),
            pltpu.VMEM((4, 256, HALF), BF16),
            pltpu.VMEM((ROWS, 512), BF16),
            pltpu.SemaphoreType.DMA((8,)),
            pltpu.SemaphoreType.DMA((4,)),
            pltpu.SemaphoreType.DMA((7,)),
            pltpu.SemaphoreType.DMA((2, 2)),
            pltpu.SemaphoreType.DMA((2, 2, 4)),
        ],
        compiler_params=pltpu.CompilerParams(
            collective_id=0, has_side_effects=True, vmem_limit_bytes=MIXER_VMEM
        ),
        name="mixer",
    )(tokens, norm_gain, in_weight, out_weight, *constants)
    return pl.pallas_call(
        finish,
        out_shape=jax.ShapeDtypeStruct((ROWS, WIDTH), BF16),
        in_specs=[vmem] * 3,
        out_specs=hbm,
        scratch_shapes=[pltpu.VMEM((8, ROWS, 512), BF16), pltpu.SemaphoreType.DMA((8,))],
        compiler_params=pltpu.CompilerParams(vmem_limit_bytes=FINISH_VMEM),
        name="finish",
    )(acc, spec_b, wmix_b)


MIXER_VMEM = 40 * 2**20
FINISH_VMEM = 8 * 2**20


def solution(mesh):
    placed = (P(("row", "col"), None), P(), P(), P())
    return jax.shard_map(
        local, mesh=mesh, in_specs=placed, out_specs=P(("row", "col"), None), check_vma=False
    )
```
